32 devices in a mesh: ep: 8 (over z, y), tp: 4 (over x, core).
Axes of the slice: x: 2, y: 2, z: 4, core: 2. Of those that a mesh axis runs over, the one named last changes fastest.
Arguments:
- conv_value: bfloat16 [4096, 2048], P('ep', 'tp'), may hold values from -6 to 6
- conv_gate: bfloat16 [4096, 2048], P('ep', 'tp'), may hold values from -9 to 9
- conv_kernel: float32 [31, 2048], P(None, 'tp'), may hold values from -20 to 20
- norm_gain: float32 [2048], P('tp'), may hold values from 0.1 to 1.9
- mixer_proj: bfloat16 [2048, 2048], P('tp'), may hold values from -0.125 to 0.125
- moe_in: bfloat16 [4096, 2048], P('ep'), may hold values from -6 to 6
- route_ids: int32 [4096, 2], P('ep'), may hold values from 0 to 7, all different within a row; in each aligned block of 128 rows (0 to 127, 128 to 255, ...) at most 64 rows name the same one
- route_logits: float32 [4096, 2], P('ep'), may hold values from -6 to 6
- moe_gain: float32 [2048], replicated, may hold values from 0.1 to 1.9
- expert_gate: bfloat16 [8, 2048, 2048], P('ep', None, 'tp'), may hold values from -0.26367188 to 0.26367188
- expert_lin: bfloat16 [8, 2048, 2048], P('ep', None, 'tp'), may hold values from -0.26367188 to 0.26367188
- expert_down: bfloat16 [8, 2048, 2048], P('ep', 'tp'), may hold values from -0.052978516 to 0.052978516
Outputs:
- mixer_out: bfloat16 [4096, 2048], P(('ep', 'tp'))
- moe_out: bfloat16 [4096, 2048], P(('ep', 'tp'))
The draws below stay inside these ranges and needn't reach their ends.
Inputs may be any that keep to these rules, and one draw needn't show every extreme that they name: `route_ids`: every row names 2 different experts. In each aligned block of 128 rows (one device's output rows) no expert is named by more than 64 rows, and in every draw some expert is named by exactly 64 rows of some block.
All inputs are finite; a program needn't handle non-finite values.
Results may differ from the reference program's by a relative error of at most 0.01.
Values may be sent and summed in bfloat16 or wider, within the bound.
A program may use at most 128 MiB of HBM per device.

```python
import math
import jax
import jax.numpy as jnp
import numpy as np
from jax import lax

D = 2048
C = 2048
F = 2048
KW = 31
TOPK = 2
ROWS = 128
EXPERTS = 8
CAP = 64
TOKM = 4096
TOKE = 4096
N_TP = 4


def draw_conv_kernel(key, part):
    first = jax.random.fold_in(key, 11)
    second = jax.random.fold_in(key, 12)
    base = jax.random.normal(first, (KW, C), jnp.float32)
    spread = jnp.exp(jax.random.uniform(second, (1, C), jnp.float32, -0.5, 0.5))
    rising = jnp.exp(math.log(10.0) * jnp.arange(C, dtype=jnp.float32) / C)[None, :]
    return base * spread * rising / math.sqrt(KW)


def levels(key, shape, pieces, low, top_value):
    factor_of, own = 1.0, jax.random.fold_in(key, 6)
    for position, shards_of in pieces:
        steps = jnp.exp(jax.random.uniform(jax.random.fold_in(own, position), (shards_of,), jnp.float32, low / len(pieces), top_value / len(pieces)))
        factor_of = factor_of * jnp.repeat(steps, shape[position] // shards_of).reshape([-1 if axis == position else 1 for axis in range(len(shape))])
    return factor_of


def routed_block(own_key, own, number, rows, count, top, bound, slope):
    order = jax.random.permutation(own_key, count)
    heavy_load, common = portions_of(count, rows * top, bound, slope, True), portions_of(count, rows * top, bound, slope, False)
    places = jnp.arange(count)

    def named(lengths, turn):
        used = int((lengths > 0).sum())
        fixed = max(1, used // 4)
        moved = fixed + (places - fixed + turn * (used - fixed)) % max(1, count - fixed)
        return jnp.zeros((count,), jnp.int32).at[order[jnp.where(places < fixed, places, moved)]].set(jnp.asarray(lengths, jnp.int32))

    lengths = jnp.where(number % 4 == 0, named(heavy_load, number // 4), named(common, number - number // 4 - 1))
    mixed = jax.random.permutation(jax.random.fold_in(own, 3), count)
    giver, sink = mixed[0:count // 2 * 2:2], mixed[1:count // 2 * 2:2]
    slack = jnp.minimum(lengths[giver] - 1, bound - lengths[sink]) // 2
    slack = jnp.where((giver == order[0]) | (sink == order[0]) | (lengths[sink] == 0), 0, jnp.maximum(slack, 0))
    moved = jax.random.randint(jax.random.fold_in(own, 4), (count // 2,), 0, 1 << 20) % (slack + 1)
    lengths = lengths.at[giver].add(-moved).at[sink].add(moved)
    items = jnp.searchsorted(jnp.cumsum(lengths), jnp.arange(rows * top), side="right").astype(jnp.int32)
    table = items.reshape(top, rows).T
    table = table[jax.random.permutation(jax.random.fold_in(own, 1), rows)]
    turn = jax.random.randint(jax.random.fold_in(own, 2), (rows, 1), 0, top)
    return jnp.take_along_axis(table, (jnp.arange(top)[None, :] + turn) % top, axis=1)


def portions_of(number_of, total, reach, skew, full):
    portions = [(1 << 20) // math.isqrt(standing ** skew) + 1 for standing in range(1, number_of + 1)]
    largest = reach if full else min(reach, max(-(-total // number_of), total * portions[0] // sum(portions)))
    least = 1 if total - largest >= number_of - 1 else 0
    given, surplus = [largest] + [least] * (number_of - 1), total - largest - least * (number_of - 1)
    while surplus > 0:
        candidates = [i for i in range(1, number_of) if given[i] < largest] or [i for i in range(1, number_of) if given[i] < reach]
        whole, remaining = sum([portions[i] for i in candidates]), surplus
        for i in candidates:
            more = min(reach - given[i], max(1, remaining * portions[i] // whole), surplus)
            given[i] = given[i] + more
            surplus = surplus - more
    return np.array(given)


def gaussian(rng, shape, width, limit, shards=(), kind=jnp.bfloat16):
    result = jax.random.normal(rng, shape, jnp.float32) * width
    if len(shards) > 0:
        result = levels(rng, shape, shards, -0.22, 0.18) * result
    return jnp.clip(result, min=-limit, max=limit).astype(kind)


def setup_inputs(seed: int = 0) -> dict:
    keys = jax.random.split(jax.random.key(seed), 13)
    conv_value = gaussian(keys[0], (TOKM, C), 1.0, 6.0, ((0, 8), (1, 4)))
    conv_gate = gaussian(keys[1], (TOKM, C), 1.5, 9.0, ((0, 8), (1, 4)))
    conv_kernel = draw_conv_kernel(jax.random.fold_in(keys[12], 71), 0)
    norm_gain = jnp.clip(1.0 + 0.18 * jax.random.normal(keys[3], (C,), jnp.float32), 0.1, 1.9)
    mixer_proj = gaussian(keys[4], (C, D), C ** -0.5, 0.125, ((0, 4),))
    moe_in = gaussian(keys[5], (TOKE, D), 1.0, 6.0, ((0, 8),))
    route_ids_keys = jax.random.split(jax.random.fold_in(keys[6], 1), TOKE // ROWS)
    route_ids_turns = jax.random.permutation(jax.random.fold_in(keys[6], 3), TOKE // ROWS)
    route_ids = jax.vmap(lambda own, number: routed_block(jax.random.fold_in(keys[6], 2), own, number, ROWS, EXPERTS, TOPK, CAP, 1))(route_ids_keys, route_ids_turns).reshape((TOKE, TOPK))
    route_logits = gaussian(keys[7], (TOKE, TOPK), 1.5, 6.0, ((0, 8),), jnp.float32)
    moe_gain = jnp.clip(1.0 + 0.18 * jax.random.normal(keys[8], (D,), jnp.float32), 0.1, 1.9)
    expert_gate = gaussian(keys[9], (EXPERTS, D, F), (2.0 * D ** -0.5), 0.26367188, ((0, 8), (2, 4)))
    expert_lin = gaussian(keys[10], (EXPERTS, D, F), (2.0 * D ** -0.5), 0.26367188, ((0, 8), (2, 4)))
    expert_down = gaussian(keys[11], (EXPERTS, F, D), (0.4 * F ** -0.5), 0.052978516, ((0, 8), (1, 4)))
    return {"conv_value": conv_value, "conv_gate": conv_gate, "conv_kernel": conv_kernel, "norm_gain": norm_gain, "mixer_proj": mixer_proj, "moe_in": moe_in, "route_ids": route_ids, "route_logits": route_logits, "moe_gain": moe_gain, "expert_gate": expert_gate, "expert_lin": expert_lin, "expert_down": expert_down}


EPS = 1e-05
LIMIT = 7.0
SLOPE = 1.702

def slot_targets(routes, experts, capacity):
    flat = routes.reshape(-1)
    onehot = (flat[:, None] == jnp.arange(experts, dtype=jnp.int32)[None, :]).astype(jnp.int32)
    rank = lax.optimization_barrier(jnp.sum(jnp.cumsum(onehot, axis=0) * onehot, axis=1)) - 1
    return (flat * capacity + rank).astype(jnp.int32)

def slot_sources(target, total, topk):
    hits = (target[None, :] == jnp.arange(total, dtype=jnp.int32)[:, None]).astype(jnp.int32)
    owner = jnp.arange(target.shape[0], dtype=jnp.int32) // topk
    source = lax.optimization_barrier(jnp.sum(hits * owner[None, :], axis=1)).astype(jnp.int32)
    filled = lax.optimization_barrier(jnp.sum(hits, axis=1)) > 0
    return (source, filled)

def reference(conv_value, conv_gate, conv_kernel, norm_gain, mixer_proj, moe_in, route_ids, route_logits, moe_gain, expert_gate, expert_lin, expert_down):
    glu = (conv_value.astype(jnp.float32) * jax.nn.sigmoid(conv_gate.astype(jnp.float32))).astype(jnp.bfloat16)
    padded = jnp.pad(glu.astype(jnp.float32), ((KW - 1, 0), (0, 0)))
    conv = jnp.zeros((TOKM, C), jnp.float32)
    for tap in range(KW):
        conv = conv + conv_kernel[tap][None, :] * padded[tap:tap + TOKM]
    mean = lax.optimization_barrier(jnp.mean(conv, axis=1, keepdims=True))
    var = lax.optimization_barrier(jnp.mean(jnp.square(conv - mean), axis=1, keepdims=True))
    conv_act = jax.nn.silu((conv - mean) * lax.rsqrt(var + EPS) * norm_gain).astype(jnp.bfloat16)
    block_c = C // N_TP
    mixer_sum = jnp.zeros((TOKM, D), jnp.float32)
    for part in range(N_TP):
        term = jnp.dot(conv_act[:, part * block_c:(part + 1) * block_c], mixer_proj[part * block_c:(part + 1) * block_c], preferred_element_type=jnp.float32)
        mixer_sum = mixer_sum + term.astype(jnp.bfloat16).astype(jnp.float32)
    mixer_out = mixer_sum.astype(jnp.bfloat16)
    xin = moe_in.astype(jnp.float32)
    mu = lax.optimization_barrier(jnp.mean(xin, axis=1, keepdims=True))
    va = lax.optimization_barrier(jnp.mean(jnp.square(xin - mu), axis=1, keepdims=True))
    moe_norm = ((xin - mu) * lax.rsqrt(va + EPS) * moe_gain).astype(jnp.bfloat16)
    blocks = TOKE // ROWS
    routes = route_ids.reshape(blocks, ROWS, TOPK)
    targets = jax.vmap(lambda r: slot_targets(r, EXPERTS, CAP))(routes)
    sources, filled = jax.vmap(lambda t: slot_sources(t, EXPERTS * CAP, TOPK))(targets)
    base = (jnp.arange(blocks, dtype=jnp.int32) * ROWS)[:, None]
    global_src = (sources + base).reshape(blocks, EXPERTS, CAP)
    live = filled.reshape(blocks, EXPERTS, CAP)
    block_f = F // N_TP

    def one_expert(expert):
        index = lax.dynamic_index_in_dim(global_src, expert, 1, keepdims=False).reshape(-1)
        mask = lax.dynamic_index_in_dim(live, expert, 1, keepdims=False).reshape(-1)
        rows = jnp.where(mask[:, None], moe_norm[index], jnp.zeros((), jnp.bfloat16))
        gate = jnp.minimum(jnp.dot(rows, expert_gate[expert], preferred_element_type=jnp.float32), LIMIT)
        lin = jnp.clip(jnp.dot(rows, expert_lin[expert], preferred_element_type=jnp.float32), -LIMIT, LIMIT)
        hidden = (gate * jax.nn.sigmoid(SLOPE * gate) * (lin + 1.0)).astype(jnp.bfloat16)
        down = expert_down[expert]
        total = jnp.zeros((rows.shape[0], D), jnp.float32)
        for part in range(N_TP):
            term = jnp.dot(hidden[:, part * block_f:(part + 1) * block_f], down[part * block_f:(part + 1) * block_f], preferred_element_type=jnp.float32)
            total = total + term.astype(jnp.bfloat16).astype(jnp.float32)
        return total.astype(jnp.bfloat16)
    outputs = lax.map(one_expert, jnp.arange(EXPERTS, dtype=jnp.int32))
    flat_out = outputs.reshape(EXPERTS * blocks * CAP, D)
    expert_id = targets // CAP
    slot = targets % CAP
    where = (expert_id * (blocks * CAP) + jnp.arange(blocks, dtype=jnp.int32)[:, None] * CAP + slot).reshape(-1)
    picked = flat_out[where].astype(jnp.float32).reshape(TOKE, TOPK, D)
    expo = jnp.exp(route_logits)
    weight = expo / lax.optimization_barrier(jnp.sum(expo, axis=1, keepdims=True))
    moe_out = lax.optimization_barrier(jnp.sum(picked * weight[:, :, None], axis=1)).astype(jnp.bfloat16)
    return (mixer_out, moe_out)
```

```python
import jax
import jax.numpy as jnp
from jax import lax
from jax.experimental import pallas as pl
from jax.experimental.pallas import tpu as pltpu
from jax.sharding import PartitionSpec as P

EPS = 1e-05
LIMIT = 7.0
SLOPE = 1.702
F32 = jnp.float32
BF16 = jnp.bfloat16


def passed_along(block, axis, distance):
    devices = range(lax.axis_size(axis))
    route = [(i - distance, i) for i in devices if i - distance in devices]
    return lax.ppermute(block, axis, route)


def slot_targets(routes, experts, capacity):
    flat = routes.reshape(-1)
    onehot = (flat[:, None] == jnp.arange(experts, dtype=jnp.int32)[None, :]).astype(jnp.int32)
    rank = jnp.sum(jnp.cumsum(onehot, axis=0) * onehot, axis=1) - 1
    return flat * capacity + rank


def remote(src, dst, send, recv, device):
    return pltpu.make_async_remote_copy(
        src_ref=src,
        dst_ref=dst,
        send_sem=send,
        recv_sem=recv,
        device_id=device,
        device_id_type=pl.DeviceIdType.MESH,
    )


def joined(block):
    groups, rows, width = block.shape
    if rows % 16:
        return block.astype(F32).reshape(groups * rows, width).astype(BF16)
    return block.reshape(groups * rows, width)


def layer_kernel(
    packed, act, wmat, gate_hbm, lin_hbm, down_hbm, proj_hbm,
    mix_out, moe_out,
    gate_w, lin_w, down_w, proj_w,
    arrived, part, a_recv, b_send, b_recv, c_send, c_recv,
    m_part, m_a, m_bs, m_b,
    load_sem, sems, m_sems,
):
    experts, cap, width = packed.shape
    rows = moe_out.shape[0]
    ep, tp = lax.axis_index("ep"), lax.axis_index("tp")
    core, side = lax.rem(tp, 2), lax.div(tp, 2)
    xpeer, cpeer = {"tp": lax.rem(tp + 2, 4)}, {"tp": tp + 1 - 2 * core}
    pos, posx = core * 2 + side, core * 2 + 1 - side
    posc, posd = (1 - core) * 2 + side, (1 - core) * 2 + 1 - side

    def chunk(d):
        return lax.rem(ep - d + experts, experts)

    def prim(d):
        e = lax.rem(ep + d, experts)
        return remote(packed.at[e], arrived.at[ep, pos], sems.at[0, d], sems.at[1, d], {"ep": e})

    def prim_in(d):
        slot = arrived.at[chunk(d), pos]
        return remote(slot, slot, sems.at[0, d], sems.at[1, d], {"ep": chunk(d)})

    own = pltpu.make_async_copy(packed.at[ep], arrived.at[ep, pos], load_sem.at[4])

    def hop(d, place, k, peer):
        slot = arrived.at[chunk(d), place]
        return remote(slot, slot, sems.at[k, d], sems.at[k + 1, d], peer)

    def xf(d):
        return hop(d, pos, 2, xpeer)

    def xf_in(d):
        return hop(d, posx, 2, xpeer)

    def cf(d):
        return hop(d, pos, 4, cpeer)

    def cf_in(d):
        return hop(d, posc, 4, cpeer)

    def cf2(d):
        return hop(d, posx, 6, cpeer)

    def cf2_in(d):
        return hop(d, posd, 6, cpeer)

    def give_a(d):
        s = chunk(d)
        return remote(part.at[s, 1 - core], a_recv.at[s], sems.at[8, d], sems.at[9, d], cpeer)

    def give_b(d):
        s = chunk(d)
        return remote(b_send.at[s], b_recv.at[s], sems.at[10, d], sems.at[11, d], xpeer)

    def give_c(d):
        s = chunk(d)
        return remote(c_send.at[s], c_recv.at[ep], sems.at[12, d], sems.at[13, d], {"ep": s})

    def give_c_in(d):
        e = lax.rem(ep + d, experts)
        return remote(c_recv.at[e], c_recv.at[e], sems.at[12, d], sems.at[13, d], {"ep": e})

    mix_a = remote(m_part.at[1 - core], m_a, m_sems.at[0], m_sems.at[1], cpeer)
    mix_b = remote(m_bs, m_b, m_sems.at[2], m_sems.at[3], xpeer)

    own.start()

    @pl.loop(1, experts)
    def _(d):
        prim(d).start()

    loads = [
        pltpu.make_async_copy(proj_hbm, proj_w, load_sem.at[3]),
        pltpu.make_async_copy(gate_hbm, gate_w, load_sem.at[0]),
        pltpu.make_async_copy(lin_hbm, lin_w, load_sem.at[1]),
        pltpu.make_async_copy(down_hbm, down_w, load_sem.at[2]),
    ]
    for load in loads:
        load.start()
    own.wait()
    xf(0).start()
    cf(0).start()

    loads[0].wait()
    for t in range(4):
        m_part[t % 2, t // 2] = jnp.dot(
            act[t * rows : (t + 1) * rows, :], proj_w[...], preferred_element_type=F32
        ).astype(BF16)
    mix_a.start()
    for load in loads[1:]:
        load.wait()

    def ffn(d):
        s = chunk(d)
        x = joined(arrived[s])
        gate = jnp.minimum(jnp.dot(x, gate_w[...], preferred_element_type=F32), LIMIT)
        lin = jnp.clip(jnp.dot(x, lin_w[...], preferred_element_type=F32), -LIMIT, LIMIT)
        hidden = (gate * jax.nn.sigmoid(SLOPE * gate) * (lin + 1.0)).astype(BF16)
        tile = min(512, width)
        for n in range(0, width, tile):
            y = jnp.dot(hidden, down_w[:, n : n + tile], preferred_element_type=F32)
            part[s, :, :, :, n : n + tile] = y.reshape(2, 2, cap, tile).astype(BF16)

    def at_step(i, lag, first=0):
        return jnp.logical_and(i - lag >= first, i - lag < experts)

    @pl.loop(0, experts + 4)
    def _(i):
        @pl.when(at_step(i, 0, 1))
        def _():
            prim_in(i).wait_recv()
            xf(i).start()
            cf(i).start()

        @pl.when(at_step(i, 1))
        def _():
            xf_in(i - 1).wait_recv()
            cf2(i - 1).start()

        @pl.when(at_step(i, 2))
        def _():
            cf_in(i - 2).wait_recv()
            cf2_in(i - 2).wait_recv()
            ffn(i - 2)
            give_a(i - 2).start()

        @pl.when(at_step(i, 3))
        def _():
            d = i - 3
            s = chunk(d)
            give_a(d).wait_recv()
            b_send[s] = (part[s, core, 1 - side].astype(F32) + a_recv[s, 1 - side].astype(F32)).astype(BF16)
            give_b(d).start()

        @pl.when(i == 3)
        def _():
            mix_a.wait_recv()
            m_bs[...] = (m_part[core, 1 - side].astype(F32) + m_a[1 - side].astype(F32)).astype(BF16)
            mix_b.start()

        @pl.when(at_step(i, 4))
        def _():
            d = i - 4
            s = chunk(d)
            give_b(d).wait_recv()
            total = part[s, core, side].astype(F32) + a_recv[s, side].astype(F32) + b_recv[s].astype(F32)

            @pl.when(d == 0)
            def _():
                c_recv[s] = total.astype(BF16)

            @pl.when(d > 0)
            def _():
                c_send[s] = total.astype(BF16)
                give_c(d).start()

    mix_b.wait_recv()
    mix_out[...] = (
        m_part[core, side].astype(F32) + m_a[side].astype(F32) + m_b[...].astype(F32)
    ).astype(BF16)

    @pl.loop(1, experts)
    def _(d):
        give_c_in(d).wait_recv()

    weight = wmat[...]
    high = weight.astype(BF16)
    low = (weight - high.astype(F32)).astype(BF16)
    tile = min(512, width)
    for n in range(0, width, tile):
        results = joined(c_recv[:, :, n : n + tile])
        moe_out[:, n : n + tile] = (
            jnp.dot(high, results, preferred_element_type=F32)
            + jnp.dot(low, results, preferred_element_type=F32)
        ).astype(BF16)

    mix_a.wait_send()
    mix_b.wait_send()

    @pl.loop(0, experts)
    def _(d):
        @pl.when(d > 0)
        def _():
            prim(d).wait_send()
            give_c(d).wait_send()

        xf(d).wait_send()
        cf(d).wait_send()
        cf2(d).wait_send()
        give_a(d).wait_send()
        give_b(d).wait_send()


def shards(
    conv_value,
    conv_gate,
    conv_kernel,
    norm_gain,
    mixer_proj,
    moe_in,
    route_ids,
    route_logits,
    moe_gain,
    expert_gate,
    expert_lin,
    expert_down,
):
    tp_size = lax.axis_size("tp")
    tp_index = lax.axis_index("tp")
    glu = (conv_value.astype(jnp.float32) * jax.nn.sigmoid(conv_gate.astype(jnp.float32))).astype(
        jnp.bfloat16
    )
    reach = conv_kernel.shape[0] - 1
    length = glu.shape[0]
    rim = passed_along(glu[length - reach :], "ep", 1)
    padded = jnp.concatenate([rim, glu], axis=0).astype(jnp.float32)
    conv = jnp.zeros(glu.shape, jnp.float32)
    for tap in range(reach + 1):
        conv = conv + conv_kernel[tap][None, :] * padded[tap : tap + length]
    total, square = lax.psum((jnp.sum(conv, axis=1), jnp.sum(conv * conv, axis=1)), "tp")
    channels = conv.shape[1] * tp_size
    mean = (total / channels)[:, None]
    var = (square / channels)[:, None] - mean * mean
    conv_act = jax.nn.silu((conv - mean) * lax.rsqrt(var + EPS) * norm_gain).astype(jnp.bfloat16)

    rows = moe_in.shape[0] // tp_size
    topk = route_ids.shape[1]
    experts = lax.axis_size("ep")
    capacity = max(2, 2 * rows * topk // experts)
    width = moe_in.shape[1]
    start = tp_index * rows
    block = lax.dynamic_slice_in_dim(moe_in, start, rows, 0).astype(jnp.float32)
    mu = jnp.mean(block, axis=1, keepdims=True)
    va = jnp.mean(jnp.square(block - mu), axis=1, keepdims=True)
    normed = ((block - mu) * lax.rsqrt(va + EPS) * moe_gain).astype(jnp.bfloat16)
    routes = lax.dynamic_slice_in_dim(route_ids, start, rows, 0)
    target = slot_targets(routes, experts, capacity).reshape(rows, topk)
    logits = lax.dynamic_slice_in_dim(route_logits, start, rows, 0)
    expo = jnp.exp(logits)
    weight = expo / jnp.sum(expo, axis=1, keepdims=True)
    slots = jnp.arange(experts * capacity, dtype=jnp.int32)
    hits = target[:, :, None] == slots[None, None, :]
    placed = jnp.any(hits, axis=1).astype(jnp.bfloat16)
    wmat = jnp.sum(jnp.where(hits, weight[:, :, None], 0.0), axis=1)
    packed = lax.dot_general(
        placed, normed, (((0,), (0,)), ((), ())), preferred_element_type=jnp.float32
    ).astype(jnp.bfloat16)
    packed = packed.reshape(experts, capacity, width)

    hid = expert_gate.shape[2]
    chans = conv_act.shape[1]
    vmem = pl.BlockSpec(memory_space=pltpu.VMEM)
    hbm = pl.BlockSpec(memory_space=pl.ANY)
    out = jax.ShapeDtypeStruct((rows, width), BF16)
    mixer_out, moe_out = pl.pallas_call(
        layer_kernel,
        out_shape=(out, out),
        in_specs=[vmem, vmem, vmem, hbm, hbm, hbm, hbm],
        out_specs=(vmem, vmem),
        scratch_shapes=[
            pltpu.VMEM((width, hid), BF16),
            pltpu.VMEM((width, hid), BF16),
            pltpu.VMEM((hid, width), BF16),
            pltpu.VMEM((chans, width), BF16),
            pltpu.VMEM((experts, tp_size, capacity, width), BF16),
            pltpu.VMEM((experts, 2, 2, capacity, width), BF16),
            pltpu.VMEM((experts, 2, capacity, width), BF16),
            pltpu.VMEM((experts, capacity, width), BF16),
            pltpu.VMEM((experts, capacity, width), BF16),
            pltpu.VMEM((experts, capacity, width), BF16),
            pltpu.VMEM((experts, capacity, width), BF16),
            pltpu.VMEM((2, 2, rows, width), BF16),
            pltpu.VMEM((2, rows, width), BF16),
            pltpu.VMEM((rows, width), BF16),
            pltpu.VMEM((rows, width), BF16),
            pltpu.SemaphoreType.DMA((5,)),
            pltpu.SemaphoreType.DMA((14, experts)),
            pltpu.SemaphoreType.DMA((4,)),
        ],
        compiler_params=pltpu.CompilerParams(
            has_side_effects=True, vmem_limit_bytes=60 * 1024 * 1024
        ),
    )(packed, conv_act, wmat, expert_gate[0], expert_lin[0], expert_down[0], mixer_proj)
    return (mixer_out, moe_out)


def solution(mesh):
    placed = (
        P("ep", "tp"),
        P("ep", "tp"),
        P(None, "tp"),
        P("tp"),
        P("tp", None),
        P("ep", None),
        P("ep", None),
        P("ep", None),
        P(),
        P("ep", None, "tp"),
        P("ep", None, "tp"),
        P("ep", "tp", None),
    )
    return jax.shard_map(
        shards,
        mesh=mesh,
        in_specs=placed,
        out_specs=(P(("ep", "tp"), None), P(("ep", "tp"), None)),
        check_vma=False,
    )
```

```python
import jax
import jax.numpy as jnp
from jax import lax
from jax.experimental import pallas as pl
from jax.experimental.pallas import tpu as pltpu
from jax.sharding import PartitionSpec as P

EPS = 1e-05
LIMIT = 7.0
SLOPE = 1.702
F32 = jnp.float32
BF16 = jnp.bfloat16


def slot_targets(routes, experts, capacity):
    flat = routes.reshape(-1)
    onehot = (flat[:, None] == jnp.arange(experts, dtype=jnp.int32)[None, :]).astype(jnp.int32)
    rank = jnp.sum(jnp.cumsum(onehot, axis=0) * onehot, axis=1) - 1
    return flat * capacity + rank


def remote(src, dst, send, recv, device):
    return pltpu.make_async_remote_copy(
        src_ref=src,
        dst_ref=dst,
        send_sem=send,
        recv_sem=recv,
        device_id=device,
        device_id_type=pl.DeviceIdType.MESH,
    )


def joined(block):
    groups, rows, width = block.shape
    if rows % 16:
        return block.astype(F32).reshape(groups * rows, width).astype(BF16)
    return block.reshape(groups * rows, width)


def layer_kernel(
    packed, wmat, value, gates, taps, gain, gate_hbm, lin_hbm, down_hbm, proj_hbm,
    mix_out, moe_out,
    gate_w, lin_w, down_w, proj_w,
    arrived, part, a_recv, b_send, b_recv, c_send, c_recv,
    m_part, m_a, m_bs, m_b,
    glu, halo, padded, conv, s_own, s_core, s_pair, s_side,
    load_sem, sems, m_sems,
):
    experts, cap, width = packed.shape
    rows = moe_out.shape[0]
    ep, tp = lax.axis_index("ep"), lax.axis_index("tp")
    core, side = lax.rem(tp, 2), lax.div(tp, 2)
    xpeer, cpeer = {"tp": lax.rem(tp + 2, 4)}, {"tp": tp + 1 - 2 * core}
    pos, posx = core * 2 + side, core * 2 + 1 - side
    posc, posd = (1 - core) * 2 + side, (1 - core) * 2 + 1 - side

    def chunk(d):
        return lax.rem(ep - d + experts, experts)

    def prim(d):
        e = lax.rem(ep + d, experts)
        return remote(packed.at[e], arrived.at[ep, pos], sems.at[0, d], sems.at[1, d], {"ep": e})

    def prim_in(d):
        slot = arrived.at[chunk(d), pos]
        return remote(slot, slot, sems.at[0, d], sems.at[1, d], {"ep": chunk(d)})

    own = pltpu.make_async_copy(packed.at[ep], arrived.at[ep, pos], load_sem.at[4])

    def hop(d, place, k, peer):
        slot = arrived.at[chunk(d), place]
        return remote(slot, slot, sems.at[k, d], sems.at[k + 1, d], peer)

    def xf(d):
        return hop(d, pos, 2, xpeer)

    def xf_in(d):
        return hop(d, posx, 2, xpeer)

    def cf(d):
        return hop(d, pos, 4, cpeer)

    def cf_in(d):
        return hop(d, posc, 4, cpeer)

    def cf2(d):
        return hop(d, posx, 6, cpeer)

    def cf2_in(d):
        return hop(d, posd, 6, cpeer)

    def give_a(d):
        s = chunk(d)
        return remote(part.at[s, 1 - core], a_recv.at[s], sems.at[8, d], sems.at[9, d], cpeer)

    def give_b(d):
        s = chunk(d)
        return remote(b_send.at[s], b_recv.at[s], sems.at[10, d], sems.at[11, d], xpeer)

    def give_c(d):
        s = chunk(d)
        return remote(c_send.at[s], c_recv.at[ep], sems.at[12, d], sems.at[13, d], {"ep": s})

    def give_c_in(d):
        e = lax.rem(ep + d, experts)
        return remote(c_recv.at[e], c_recv.at[e], sems.at[12, d], sems.at[13, d], {"ep": e})

    mix_a = remote(m_part.at[1 - core], m_a, m_sems.at[0], m_sems.at[1], cpeer)
    mix_b = remote(m_bs, m_b, m_sems.at[2], m_sems.at[3], xpeer)

    length, rim = glu.shape[0], halo.shape[0]
    reach = taps.shape[0] - 1
    channels = glu.shape[1] * 4
    forward = lax.rem(ep + 1, experts)
    edge = remote(glu.at[pl.ds(length - rim, rim)], halo, m_sems.at[4], m_sems.at[5], {"ep": forward})
    stat_a = remote(s_own, s_core, m_sems.at[6], m_sems.at[7], cpeer)
    stat_b = remote(s_pair, s_side, m_sems.at[8], m_sems.at[9], xpeer)

    def gated():
        glu[...] = (value[...].astype(F32) * jax.nn.sigmoid(gates[...].astype(F32))).astype(BF16)

        @pl.when(ep < experts - 1)
        def _():
            edge.start()

        padded[rim:, :] = glu[...].astype(F32)

    def convolved():
        @pl.when(ep > 0)
        def _():
            edge.wait_recv()
            padded[:rim, :] = halo[...].astype(F32)

        @pl.when(ep == 0)
        def _():
            padded[:rim, :] = jnp.zeros((rim, padded.shape[1]), F32)

        step = min(64, length)

        @pl.loop(0, glu.shape[1] // 128)
        def _(j):
            lanes = pl.ds(pl.multiple_of(j * 128, 128), 128)
            for r in range(0, length, step):
                total = jnp.zeros((step, 128), F32)
                for tap in range(reach + 1):
                    first = r + rim - reach + tap
                    total = total + taps[tap : tap + 1, lanes] * padded[first : first + step, lanes]
                conv[r : r + step, lanes] = total

        full = conv[...]
        lane = lax.broadcasted_iota(jnp.int32, s_own.shape, 1)
        s_own[...] = jnp.where(
            lane == 0,
            jnp.sum(full, axis=1, keepdims=True),
            jnp.where(lane == 1, jnp.sum(full * full, axis=1, keepdims=True), 0.0),
        )
        stat_a.start()

    def paired():
        stat_a.wait_recv()
        s_pair[...] = s_own[...] + s_core[...]
        stat_b.start()

    def projected():
        stat_b.wait_recv()
        for t in range(4):
            own_rows = slice(t * rows, (t + 1) * rows)
            stats = s_pair[own_rows, :] + s_side[own_rows, :]
            mean = stats[:, 0:1] / channels
            var = stats[:, 1:2] / channels - mean * mean
            act = jax.nn.silu((conv[own_rows, :] - mean) * lax.rsqrt(var + EPS) * gain[...]).astype(BF16)
            m_part[t % 2, t // 2] = jnp.dot(act, proj_w[...], preferred_element_type=F32).astype(BF16)
        mix_a.start()

    own.start()

    @pl.loop(1, experts)
    def _(d):
        prim(d).start()

    loads = [
        pltpu.make_async_copy(proj_hbm, proj_w, load_sem.at[3]),
        pltpu.make_async_copy(gate_hbm, gate_w, load_sem.at[0]),
        pltpu.make_async_copy(lin_hbm, lin_w, load_sem.at[1]),
        pltpu.make_async_copy(down_hbm, down_w, load_sem.at[2]),
    ]
    for load in loads:
        load.start()
    own.wait()
    xf(0).start()
    cf(0).start()

    gated()
    for load in loads:
        load.wait()

    def ffn(d):
        s = chunk(d)
        x = joined(arrived[s])
        gate = jnp.minimum(jnp.dot(x, gate_w[...], preferred_element_type=F32), LIMIT)
        lin = jnp.clip(jnp.dot(x, lin_w[...], preferred_element_type=F32), -LIMIT, LIMIT)
        hidden = (gate * jax.nn.sigmoid(SLOPE * gate) * (lin + 1.0)).astype(BF16)
        tile = min(512, width)
        for n in range(0, width, tile):
            y = jnp.dot(hidden, down_w[:, n : n + tile], preferred_element_type=F32)
            part[s, :, :, :, n : n + tile] = y.reshape(2, 2, cap, tile).astype(BF16)

    def at_step(i, lag, first=0):
        return jnp.logical_and(i - lag >= first, i - lag < experts)

    @pl.loop(0, experts + 4)
    def _(i):
        @pl.when(at_step(i, 0, 1))
        def _():
            prim_in(i).wait_recv()
            xf(i).start()
            cf(i).start()

        @pl.when(at_step(i, 1))
        def _():
            xf_in(i - 1).wait_recv()
            cf2(i - 1).start()

        @pl.when(at_step(i, 2))
        def _():
            cf_in(i - 2).wait_recv()
            cf2_in(i - 2).wait_recv()
            ffn(i - 2)
            give_a(i - 2).start()

        @pl.when(at_step(i, 3))
        def _():
            d = i - 3
            s = chunk(d)
            give_a(d).wait_recv()
            b_send[s] = (part[s, core, 1 - side].astype(F32) + a_recv[s, 1 - side].astype(F32)).astype(BF16)
            give_b(d).start()

        @pl.when(i == 1)
        def _():
            convolved()

        @pl.when(i == 2)
        def _():
            paired()

        @pl.when(i == 3)
        def _():
            projected()

        @pl.when(i == 4)
        def _():
            mix_a.wait_recv()
            m_bs[...] = (m_part[core, 1 - side].astype(F32) + m_a[1 - side].astype(F32)).astype(BF16)
            mix_b.start()

        @pl.when(at_step(i, 4))
        def _():
            d = i - 4
            s = chunk(d)
            give_b(d).wait_recv()
            total = part[s, core, side].astype(F32) + a_recv[s, side].astype(F32) + b_recv[s].astype(F32)

            @pl.when(d == 0)
            def _():
                c_recv[s] = total.astype(BF16)

            @pl.when(d > 0)
            def _():
                c_send[s] = total.astype(BF16)
                give_c(d).start()

    mix_b.wait_recv()
    mix_out[...] = (
        m_part[core, side].astype(F32) + m_a[side].astype(F32) + m_b[...].astype(F32)
    ).astype(BF16)

    @pl.loop(1, experts)
    def _(d):
        give_c_in(d).wait_recv()

    weight = wmat[...]
    high = weight.astype(BF16)
    low = (weight - high.astype(F32)).astype(BF16)
    tile = min(512, width)
    for n in range(0, width, tile):
        results = joined(c_recv[:, :, n : n + tile])
        moe_out[:, n : n + tile] = (
            jnp.dot(high, results, preferred_element_type=F32)
            + jnp.dot(low, results, preferred_element_type=F32)
        ).astype(BF16)

    @pl.when(ep < experts - 1)
    def _():
        edge.wait_send()

    stat_a.wait_send()
    stat_b.wait_send()
    mix_a.wait_send()
    mix_b.wait_send()

    @pl.loop(0, experts)
    def _(d):
        @pl.when(d > 0)
        def _():
            prim(d).wait_send()
            give_c(d).wait_send()

        xf(d).wait_send()
        cf(d).wait_send()
        cf2(d).wait_send()
        give_a(d).wait_send()
        give_b(d).wait_send()


def shards(
    conv_value,
    conv_gate,
    conv_kernel,
    norm_gain,
    mixer_proj,
    moe_in,
    route_ids,
    route_logits,
    moe_gain,
    expert_gate,
    expert_lin,
    expert_down,
):
    tp_size = lax.axis_size("tp")
    tp_index = lax.axis_index("tp")
    rows = moe_in.shape[0] // tp_size
    topk = route_ids.shape[1]
    experts = lax.axis_size("ep")
    capacity = max(2, 2 * rows * topk // experts)
    width = moe_in.shape[1]
    start = tp_index * rows
    block = lax.dynamic_slice_in_dim(moe_in, start, rows, 0).astype(jnp.float32)
    mu = jnp.mean(block, axis=1, keepdims=True)
    va = jnp.mean(jnp.square(block - mu), axis=1, keepdims=True)
    normed = ((block - mu) * lax.rsqrt(va + EPS) * moe_gain).astype(jnp.bfloat16)
    routes = lax.dynamic_slice_in_dim(route_ids, start, rows, 0)
    target = slot_targets(routes, experts, capacity).reshape(rows, topk)
    logits = lax.dynamic_slice_in_dim(route_logits, start, rows, 0)
    expo = jnp.exp(logits)
    weight = expo / jnp.sum(expo, axis=1, keepdims=True)
    slots = jnp.arange(experts * capacity, dtype=jnp.int32)
    hits = target[:, :, None] == slots[None, None, :]
    placed = jnp.any(hits, axis=1).astype(jnp.bfloat16)
    wmat = jnp.sum(jnp.where(hits, weight[:, :, None], 0.0), axis=1)
    packed = lax.dot_general(
        placed, normed, (((0,), (0,)), ((), ())), preferred_element_type=jnp.float32
    ).astype(jnp.bfloat16)
    packed = packed.reshape(experts, capacity, width)

    hid = expert_gate.shape[2]
    length, chans = conv_value.shape
    rim = -(-(conv_kernel.shape[0] - 1) // 16) * 16
    vmem = pl.BlockSpec(memory_space=pltpu.VMEM)
    hbm = pl.BlockSpec(memory_space=pl.ANY)
    out = jax.ShapeDtypeStruct((rows, width), BF16)
    mixer_out, moe_out = pl.pallas_call(
        layer_kernel,
        out_shape=(out, out),
        in_specs=[vmem] * 6 + [hbm, hbm, hbm, hbm],
        out_specs=(vmem, vmem),
        scratch_shapes=[
            pltpu.VMEM((width, hid), BF16),
            pltpu.VMEM((width, hid), BF16),
            pltpu.VMEM((hid, width), BF16),
            pltpu.VMEM((chans, width), BF16),
            pltpu.VMEM((experts, tp_size, capacity, width), BF16),
            pltpu.VMEM((experts, 2, 2, capacity, width), BF16),
            pltpu.VMEM((experts, 2, capacity, width), BF16),
            pltpu.VMEM((experts, capacity, width), BF16),
            pltpu.VMEM((experts, capacity, width), BF16),
            pltpu.VMEM((experts, capacity, width), BF16),
            pltpu.VMEM((experts, capacity, width), BF16),
            pltpu.VMEM((2, 2, rows, width), BF16),
            pltpu.VMEM((2, rows, width), BF16),
            pltpu.VMEM((rows, width), BF16),
            pltpu.VMEM((rows, width), BF16),
            pltpu.VMEM((length, chans), BF16),
            pltpu.VMEM((rim, chans), BF16),
            pltpu.VMEM((rim + length, chans), F32),
            pltpu.VMEM((length, chans), F32),
            pltpu.VMEM((length, 128), F32),
            pltpu.VMEM((length, 128), F32),
            pltpu.VMEM((length, 128), F32),
            pltpu.VMEM((length, 128), F32),
            pltpu.SemaphoreType.DMA((5,)),
            pltpu.SemaphoreType.DMA((14, experts)),
            pltpu.SemaphoreType.DMA((10,)),
        ],
        compiler_params=pltpu.CompilerParams(
            has_side_effects=True, vmem_limit_bytes=60 * 1024 * 1024
        ),
    )(
        packed, wmat, conv_value, conv_gate, conv_kernel, norm_gain[None, :],
        expert_gate[0], expert_lin[0], expert_down[0], mixer_proj,
    )
    return (mixer_out, moe_out)


def solution(mesh):
    placed = (
        P("ep", "tp"),
        P("ep", "tp"),
        P(None, "tp"),
        P("tp"),
        P("tp", None),
        P("ep", None),
        P("ep", None),
        P("ep", None),
        P(),
        P("ep", None, "tp"),
        P("ep", None, "tp"),
        P("ep", "tp", None),
    )
    return jax.shard_map(
        shards,
        mesh=mesh,
        in_specs=placed,
        out_specs=(P(("ep", "tp"), None), P(("ep", "tp"), None)),
        check_vma=False,
    )
```
